32 devices in a mesh: sp: 8 (over z, x), tp: 4 (over y, core).
Axes of the slice: x: 2, y: 2, z: 4, core: 2. Of those that a mesh axis runs over, the one named last changes fastest.
Arguments:
- target_rows: bfloat16 [512, 2048], P(('sp', 'tp')), may hold values from -6 to 6
- source_rows: bfloat16 [2048, 2048], P(('sp', 'tp')), may hold values from -6 to 6
- norm_gain: bfloat16 [2048], replicated, may hold values from 0.099609375 to 1.8984375
- query_weight: bfloat16 [2048, 4096], P(None, 'tp'), may hold values from -0.125 to 0.125
- key_weight: bfloat16 [2048, 4096], P(None, 'tp'), may hold values from -0.125 to 0.125
- value_weight: bfloat16 [2048, 4096], P(None, 'tp'), may hold values from -0.125 to 0.125
- output_weight: bfloat16 [4096, 2048], P('tp'), may hold values from -0.09375 to 0.09375
- saved_output: bfloat16 [512, 4096], P('sp', 'tp'), may hold values from -3 to 3
- norm_offset: bfloat16 [512, 16], P('sp', 'tp'), may hold values from 0.25 to 1.25
- output_grad: bfloat16 [512, 2048], P(('sp', 'tp')), may hold values from -192 to 192
Outputs:
- target_grad: float32 [512, 2048], P(('sp', 'tp'))
- source_grad: float32 [2048, 2048], P(('sp', 'tp'))
- query_weight_grad: float32 [2048, 4096], P('sp', 'tp')
The draws below stay inside these ranges and needn't reach their ends.
All inputs are finite; a program needn't handle non-finite values.
Results may differ from the reference program's by a relative error of at most 0.033.
Values may be sent and summed in bfloat16 or wider, within the bound.
A program may use at most 64 MiB of HBM per device.

```python
import math
import jax
import jax.numpy as jnp
from jax import lax

D = 2048
HEADS = 16
HEAD_DIM = 256
TARGET = 512
SOURCE = 2048


def block_scale(rng, dims, pieces, low, top_value):
    def one(axis_at, shards_of):
        steps = jax.random.uniform(jax.random.fold_in(jax.random.fold_in(rng, 6), axis_at), (shards_of,), jnp.float32, low / len(pieces), top_value / len(pieces))
        return jnp.repeat(jnp.exp(steps), dims[axis_at] // shards_of).reshape((-1,) + (1,) * (len(dims) - axis_at - 1))

    factor_of = one(*pieces[0])
    for cut in pieces[1:]:
        factor_of = factor_of * one(*cut)
    return factor_of


def bell_draw(key, extent, scale, bound, cuts=(), kind=jnp.bfloat16):
    values = jax.random.normal(key, extent, jnp.float32) * scale
    if len(cuts) > 0:
        values = block_scale(key, extent, cuts, -0.22, 0.18) * values
    return jnp.clip(values, min=-bound, max=bound).astype(kind)


def setup_inputs(seed: int = 0) -> dict:
    streams_of = jax.random.split(jax.random.key(seed), 11)
    target_rows = bell_draw(streams_of[0], (TARGET, D), 1.0, 6.0, ((0, 32),))
    source_rows = bell_draw(streams_of[1], (SOURCE, D), 1.0, 6.0, ((0, 32),))
    norm_gain = jnp.clip(1.0 + 0.18 * jax.random.normal(streams_of[2], (D,), jnp.float32), 0.099609375, 1.8984375).astype(jnp.bfloat16)
    query_weight = bell_draw(streams_of[3], (D, HEADS * HEAD_DIM), D ** -0.5, 0.125, ((1, 4),))
    key_weight = bell_draw(streams_of[4], (D, HEADS * HEAD_DIM), D ** -0.5, 0.125, ((1, 4),))
    value_weight = bell_draw(streams_of[5], (D, HEADS * HEAD_DIM), D ** -0.5, 0.125, ((1, 4),))
    output_weight = bell_draw(streams_of[6], (HEADS * HEAD_DIM, D), (HEADS * HEAD_DIM) ** -0.5, 0.09375, ((0, 4),))
    saved_output = bell_draw(streams_of[7], (TARGET, HEADS * HEAD_DIM), 0.5, 3.0, ((0, 8), (1, 4)))
    norm_offset = jnp.clip(0.25 + 1.0 * jax.random.uniform(streams_of[8], (TARGET, HEADS), jnp.float32) ** block_scale(streams_of[8], (TARGET, HEADS), ((0, 8), (1, 4)), -0.2, 0.2), 0.25, 1.25).astype(jnp.bfloat16)
    output_grad = bell_draw(streams_of[9], (TARGET, D), 32.0, 192.0, ((0, 32),))
    return {"target_rows": target_rows, "source_rows": source_rows, "norm_gain": norm_gain, "query_weight": query_weight, "key_weight": key_weight, "value_weight": value_weight, "output_weight": output_weight, "saved_output": saved_output, "norm_offset": norm_offset, "output_grad": output_grad}


EPSILON = 1e-06

def head_grads(operands):
    query_rows, head_gradient, shifts, deltas, key_row_block, value_row_block = operands
    score_scale = HEAD_DIM ** (-0.5)
    score_matrix = jnp.dot(query_rows, key_row_block.T, preferred_element_type=jnp.float32)
    prob_rows = jnp.exp(score_matrix * score_scale - shifts[:, None])
    prob_grad = jnp.dot(head_gradient, value_row_block.T, preferred_element_type=jnp.float32)
    score_grad = prob_rows * (prob_grad - deltas.astype(jnp.float32)[:, None]) * score_scale
    probability_rounded = prob_rows.astype(jnp.bfloat16)
    score_rounded = score_grad.astype(jnp.bfloat16)
    query_grad = jnp.dot(score_rounded, key_row_block, preferred_element_type=jnp.float32)
    key_grad = jnp.dot(score_rounded.T, query_rows, preferred_element_type=jnp.float32)
    value_grad = jnp.dot(probability_rounded.T, head_gradient, preferred_element_type=jnp.float32)
    return (query_grad, key_grad, value_grad)

def by_head(array, row_count):
    return array.reshape(row_count, HEADS, HEAD_DIM).transpose(1, 0, 2)

def from_head(array, row_count):
    return array.transpose(1, 0, 2).reshape(row_count, HEADS * HEAD_DIM)

def reference(target_rows, source_rows, norm_gain, query_weight, key_weight, value_weight, output_weight, saved_output, norm_offset, output_grad):
    target_float = target_rows.astype(jnp.float32)
    gain_float = norm_gain.astype(jnp.float32)
    inverse = lax.rsqrt(lax.optimization_barrier(jnp.mean(target_float * target_float, axis=1, keepdims=True)) + EPSILON)
    normed = (target_float * inverse * gain_float).astype(jnp.bfloat16)
    query_rows = jnp.dot(normed, query_weight, preferred_element_type=jnp.float32).astype(jnp.bfloat16)
    key_row_block = jnp.dot(source_rows, key_weight, preferred_element_type=jnp.float32).astype(jnp.bfloat16)
    value_row_block = jnp.dot(source_rows, value_weight, preferred_element_type=jnp.float32).astype(jnp.bfloat16)
    head_gradient = jnp.dot(output_grad, output_weight.T, preferred_element_type=jnp.float32).astype(jnp.bfloat16)
    products = head_gradient.astype(jnp.float32) * saved_output.astype(jnp.float32)
    deltas = lax.optimization_barrier(jnp.sum(products.reshape(TARGET, HEADS, HEAD_DIM), axis=2)).astype(jnp.bfloat16)
    shifts = (math.log(SOURCE) + norm_offset.astype(jnp.float32)).T
    outputs = lax.map(head_grads, (by_head(query_rows, TARGET), by_head(head_gradient, TARGET), shifts, deltas.T, by_head(key_row_block, SOURCE), by_head(value_row_block, SOURCE)))
    query_flat = from_head(outputs[0].astype(jnp.bfloat16), TARGET)
    key_flat = from_head(outputs[1].astype(jnp.bfloat16), SOURCE)
    value_flat = from_head(outputs[2].astype(jnp.bfloat16), SOURCE)
    normed_grad = jnp.dot(query_flat, query_weight.T, preferred_element_type=jnp.float32)
    scaled = normed_grad * gain_float
    target_grad = inverse * scaled - target_float * inverse ** 3 * lax.optimization_barrier(jnp.mean(scaled * target_float, axis=1, keepdims=True))
    source_grad = jnp.dot(key_flat, key_weight.T, preferred_element_type=jnp.float32) + jnp.dot(value_flat, value_weight.T, preferred_element_type=jnp.float32)
    weight_grad = jnp.dot(normed.T, query_flat, preferred_element_type=jnp.float32)
    return (target_grad, source_grad, weight_grad)
```

```python
import functools
import math

import jax
import jax.numpy as jnp
from jax import lax
from jax.experimental import pallas as pl
from jax.experimental.pallas import tpu as pltpu
from jax.sharding import PartitionSpec as P

HEAD_DIM = 256
EPSILON = 1e-06
MESH = pl.DeviceIdType.MESH
BF = jnp.bfloat16
F32 = jnp.float32
VMEM = pl.BlockSpec(memory_space=pltpu.VMEM)


def contract_last(left, right):
    return lax.dot_general(left, right, (((1,), (1,)), ((), ())), preferred_element_type=F32)


def push(src, dst, send, recv, device):
    return pltpu.make_async_remote_copy(
        src_ref=src, dst_ref=dst, send_sem=send, recv_sem=recv, device_id=device, device_id_type=MESH
    )


def greet(devices):
    barrier = pltpu.get_barrier_semaphore()
    for device in devices:
        pl.semaphore_signal(barrier, inc=1, device_id=device, device_id_type=MESH)
    pl.semaphore_wait(barrier, len(devices))


class Place:
    def __init__(self, sp, tp):
        self.sp, self.tp, self.Z, self.Y = sp, tp, sp // 2, tp // 2
        self.s, self.t = lax.axis_index("sp"), lax.axis_index("tp")
        self.z, self.x = self.s // 2, self.s % 2
        self.y, self.c = self.t // 2, self.t % 2
        self.partner = (self.s, self.y * 2 + 1 - self.c)
        self.across = (self.z * 2 + 1 - self.x, self.t)

    def chip_y(self, d):
        return (self.s, lax.rem(self.y + d + self.Y, self.Y) * 2 + self.c)

    def chip_z(self, d):
        return (lax.rem(self.z + d + self.Z, self.Z) * 2 + self.x, self.t)


class LineGather:
    def __init__(self, place, pairs, up_s, up_r, dn_s, dn_r, x_s, x_r):
        self.p, self.pairs = place, pairs
        self.sems = (up_s, up_r, dn_s, dn_r, x_s, x_r)

    def up(self, n, d, own=False):
        p, (own_ref, all_ref) = self.p, self.pairs[n]
        block = p.s - 2 * (d - 1)
        src = own_ref if own else all_ref.at[block]
        return push(src, all_ref.at[block], self.sems[0].at[n, d], self.sems[1].at[n, d], (p.s + 2, p.t))

    def up_wait(self, n, d):
        p, (_, all_ref) = self.p, self.pairs[n]
        ref = all_ref.at[p.s - 2 * d]
        return push(ref, ref, self.sems[0].at[n, d], self.sems[1].at[n, d], (p.s - 2, p.t))

    def dn(self, n, d, own=False):
        p, (own_ref, all_ref) = self.p, self.pairs[n]
        block = p.s + 2 * (d - 1)
        src = own_ref if own else all_ref.at[block]
        return push(src, all_ref.at[block], self.sems[2].at[n, d], self.sems[3].at[n, d], (p.s - 2, p.t))

    def dn_wait(self, n, d):
        p, (_, all_ref) = self.p, self.pairs[n]
        ref = all_ref.at[p.s + 2 * d]
        return push(ref, ref, self.sems[2].at[n, d], self.sems[3].at[n, d], (p.s + 2, p.t))

    def over(self, n, d):
        p, (own_ref, all_ref) = self.p, self.pairs[n]
        block = p.s - 2 * d
        k = d + p.Z - 1
        src = own_ref if d == 0 else all_ref.at[block]
        return push(src, all_ref.at[block], self.sems[4].at[n, k], self.sems[5].at[n, k], p.across)

    def over_wait(self, n, d):
        p, (_, all_ref) = self.p, self.pairs[n]
        ref = all_ref.at[p.z * 2 + 1 - p.x - 2 * d]
        k = d + p.Z - 1
        return push(ref, ref, self.sems[4].at[n, k], self.sems[5].at[n, k], p.across)

    def start(self):
        p = self.p
        count = range(len(self.pairs))

        @pl.when(p.z + 1 < p.Z)
        def _():
            for n in count:
                self.up(n, 1, True).start()

        @pl.when(p.z >= 1)
        def _():
            for n in count:
                self.dn(n, 1, True).start()

        for n in count:
            self.over(n, 0).start()

    def step(self, d):
        p = self.p
        for n in range(len(self.pairs)):

            @pl.when(p.z - d >= 0)
            def _():
                self.up_wait(n, d).wait_recv()

                @pl.when(p.z + 1 < p.Z)
                def _():
                    self.up(n, d + 1).start()

                self.over(n, d).start()

            @pl.when(p.z + d < p.Z)
            def _():
                self.dn_wait(n, d).wait_recv()

                @pl.when(p.z >= 1)
                def _():
                    self.dn(n, d + 1).start()

                self.over(n, -d).start()

    def finish(self):
        p = self.p
        for n in range(len(self.pairs)):
            for d in range(p.Z):
                for sign in (1, -1) if d else (1,):

                    @pl.when((p.z - d >= 0) if sign > 0 else (p.z + d < p.Z))
                    def _():
                        self.over_wait(n, sign * d).wait_recv()
                        self.over(n, sign * d).wait_send()

            for d in range(1, p.Z):

                @pl.when(jnp.logical_and(p.z - d + 1 >= 0, p.z + 1 < p.Z))
                def _():
                    self.up(n, d).wait_send()

                @pl.when(jnp.logical_and(p.z + d - 1 < p.Z, p.z >= 1))
                def _():
                    self.dn(n, d).wait_send()


def line_sems(p_z, n):
    return [pltpu.SemaphoreType.DMA((n, p_z + 1))] * 4 + [pltpu.SemaphoreType.DMA((n, 2 * p_z))] * 2


def rows_kernel(sp, tp, tgt, src, pieces, tgt_all, src_all, cols, loc, ys, yr, ps, pr, es, er):
    p = Place(sp, tp)
    greet(
        [p.partner]
        + [p.chip_y(d) for d in range(1, p.Y)]
        + [(lax.rem(p.s + e, sp), p.t) for e in range(1, sp)]
    )

    def spot(t, j):
        if j == 0:
            return tgt_all.at[:, t]
        return src_all.at[t]

    own = (tgt, src)
    started = []
    for j in range(2):
        for d in range(1, p.Y):
            copy = push(own[j], spot(p.t, j), ys.at[j, d], yr.at[j, d], p.chip_y(d))
            copy.start()
            started.append(copy)
        copy = push(own[j], spot(p.t, j), ps.at[j, 0], pr.at[j, 0], p.partner)
        copy.start()
        started.append(copy)
    for e in range(1, sp):
        s = lax.rem(p.s + e, sp)
        copy = push(pieces.at[s], cols.at[p.s], es.at[e], er.at[e], (s, p.t))
        copy.start()
        started.append(copy)
    mine = [
        pltpu.make_async_copy(tgt, spot(p.t, 0), loc.at[0]),
        pltpu.make_async_copy(src, spot(p.t, 1), loc.at[1]),
        pltpu.make_async_copy(pieces.at[p.s], cols.at[p.s], loc.at[2]),
    ]
    for copy in mine:
        copy.start()
    for j in range(2):
        for d in range(1, p.Y):
            t = lax.rem(p.y - d + p.Y, p.Y) * 2 + p.c
            ref = spot(t, j)
            push(ref, ref, ys.at[j, d], yr.at[j, d], p.chip_y(-d)).wait_recv()
            copy = push(ref, ref, ps.at[j, d], pr.at[j, d], p.partner)
            copy.start()
            started.append(copy)
    for j in range(2):
        for d in range(p.Y):
            ref = spot(lax.rem(p.y - d + p.Y, p.Y) * 2 + 1 - p.c, j)
            push(ref, ref, ps.at[j, d], pr.at[j, d], p.partner).wait_recv()
    for e in range(1, sp):
        s = lax.rem(p.s - e + sp, sp)
        push(cols.at[s], cols.at[s], es.at[e], er.at[e], (s, p.t)).wait_recv()
    for copy in started:
        copy.wait_send()
    for copy in mine:
        copy.wait()


def heads_kernel(
    sp, tp, q, hg, small, cols, q_all, hg_all, small_all, cols_all, loc, ys, yr, ps, pr, *line
):
    p = Place(sp, tp)
    greet(
        [p.partner, p.across]
        + [p.chip_y(d) for d in range(1, p.Y)]
        + [p.chip_z(d) for d in range(1, p.Z)]
    )
    gather = LineGather(p, ((q, q_all), (hg, hg_all), (small, small_all)), *line)
    gather.start()
    started = []
    for d in range(1, p.Y):
        copy = push(cols, cols_all.at[:, p.t], ys.at[d], yr.at[d], p.chip_y(d))
        copy.start()
        started.append(copy)
    copy = push(cols, cols_all.at[:, p.t], ps.at[0], pr.at[0], p.partner)
    copy.start()
    started.append(copy)
    mine = [
        pltpu.make_async_copy(q, q_all.at[p.s], loc.at[0]),
        pltpu.make_async_copy(hg, hg_all.at[p.s], loc.at[1]),
        pltpu.make_async_copy(small, small_all.at[p.s], loc.at[2]),
        pltpu.make_async_copy(cols, cols_all.at[:, p.t], loc.at[3]),
    ]
    for copy in mine:
        copy.start()
    for d in range(1, p.Z):
        gather.step(d)
        if d == 1:
            for k in range(1, p.Y):
                ref = cols_all.at[:, lax.rem(p.y - k + p.Y, p.Y) * 2 + p.c]
                push(ref, ref, ys.at[k], yr.at[k], p.chip_y(-k)).wait_recv()
                copy = push(ref, ref, ps.at[k], pr.at[k], p.partner)
                copy.start()
                started.append(copy)
    for k in range(p.Y):
        ref = cols_all.at[:, lax.rem(p.y - k + p.Y, p.Y) * 2 + 1 - p.c]
        push(ref, ref, ps.at[k], pr.at[k], p.partner).wait_recv()
    gather.finish()
    for copy in started:
        copy.wait_send()
    for copy in mine:
        copy.wait()


class PairScatter:
    def __init__(self, p, part, first, summed, second, fs, fr, ss, sr):
        self.p, self.part, self.first, self.summed, self.second = p, part, first, summed, second
        self.sems = (fs, fr, ss, sr)
        self.started = []

    def start(self):
        p = self.p
        for d in range(p.Y):
            y = lax.rem(p.y + d, p.Y)
            copy = push(
                self.part(y * 2 + 1 - p.c), self.first.at[d], self.sems[0].at[d], self.sems[1].at[d], p.partner
            )
            copy.start()
            self.started.append(copy)

    def middle(self):
        p = self.p
        for d in list(range(1, p.Y)) + [0]:
            y = lax.rem(p.y + d, p.Y)
            self.started[d].wait_recv()
            total = self.part(y * 2 + p.c)[...].astype(F32) + self.first[d].astype(F32)
            self.summed[d] = total.astype(BF)
            if d:
                copy = push(
                    self.summed.at[d], self.second.at[d], self.sems[2].at[d], self.sems[3].at[d], p.chip_y(d)
                )
                copy.start()
                self.started.append(copy)

    def finish(self):
        p = self.p
        total = self.part(p.t)[...].astype(F32) + self.first[0].astype(F32)
        for d in range(1, p.Y):
            self.started[p.Y + d - 1].wait_recv()
            total = total + self.second[d].astype(F32)
        for copy in self.started:
            copy.wait_send()
        return total


def grads_kernel(
    sp, tp, part, sg, wq, q_all, src_out, ng_out,
    xr, xz, zr, sg1, sg2, sg3, ng, ng1, ng2, ng3,
    xs_s, xs_r, zs_s, zs_r, a0, a1, a2, a3, b0, b1, b2, b3, *line
):
    p = Place(sp, tp)
    rows = ng1.shape[1]
    greet(
        [p.partner, p.across]
        + [p.chip_y(d) for d in range(1, p.Y)]
        + [p.chip_z(d) for d in range(1, p.Z)]
    )
    started = []
    order = list(range(1, p.Z)) + [0]
    into = {}
    for k in order:
        z = lax.rem(p.z + k, p.Z)
        into[k] = push(part.at[z * 2 + 1 - p.x], xr.at[k], xs_s.at[k], xs_r.at[k], p.across)
        into[k].start()
    source = PairScatter(p, lambda t: sg.at[t], sg1, sg2, sg3, a0, a1, a2, a3)
    source.start()
    source.middle()
    hops = {}
    for k in order[:-1]:
        into[k].wait_recv()
        z = lax.rem(p.z + k, p.Z)
        xz[k] = (part[z * 2 + p.x].astype(F32) + xr[k].astype(F32)).astype(BF)
        hops[k] = push(xz.at[k], zr.at[k], zs_s.at[k], zs_r.at[k], p.chip_z(k))
        hops[k].start()
    into[0].wait_recv()
    total = part[p.s].astype(F32) + xr[0].astype(F32)
    for k in order[:-1]:
        hops[k].wait_recv()
        total = total + zr[k].astype(F32)
    q_all[p.s] = total.astype(BF)
    gather = LineGather(p, ((q_all.at[p.s], q_all),), *line)
    gather.start()
    flat = total.astype(BF)
    width = wq.shape[0]
    tile = min(width, 256)
    for j in range(0, width, tile):
        columns = contract_last(flat, wq[j : j + tile, :]).astype(BF)
        for t in range(tp):
            ng[t, :, j : j + tile] = columns[t * rows : (t + 1) * rows]
    normed = PairScatter(p, lambda t: ng.at[t], ng1, ng2, ng3, b0, b1, b2, b3)
    normed.start()
    for d in range(1, p.Z):
        gather.step(d)
        if d == 1:
            normed.middle()
    src_out[...] = source.finish()
    ng_out[...] = normed.finish()
    gather.finish()
    for k in order:
        into[k].wait_send()
    for k in order[:-1]:
        hops[k].wait_send()


def call(kernel, name, cid, outs, scratch, *args):
    return pl.pallas_call(
        kernel,
        out_shape=[jax.ShapeDtypeStruct(*o) for o in outs],
        in_specs=[VMEM] * len(args),
        out_specs=[VMEM] * len(outs),
        scratch_shapes=scratch,
        name=name,
        compiler_params=pltpu.CompilerParams(
            collective_id=cid, has_side_effects=True, vmem_limit_bytes=56 * 2**20
        ),
    )(*args)


def body(
    target_rows,
    source_rows,
    norm_gain,
    query_weight,
    key_weight,
    value_weight,
    output_weight,
    saved_output,
    norm_offset,
    output_grad,
):
    tp, sp = lax.axis_size("tp"), lax.axis_size("sp")
    Z, Y = sp // 2, tp // 2
    model, width = query_weight.shape
    heads = width // HEAD_DIM
    rows, srows = target_rows.shape[0], source_rows.shape[0]
    block = rows * tp
    count = block * sp
    source_count = srows * tp
    shift_base = math.log(source_count * sp)
    slice_width = model // sp
    dma = pltpu.SemaphoreType.DMA
    scale = HEAD_DIM ** (-0.5)

    target_float = target_rows.astype(F32)
    gain_float = norm_gain.astype(F32)
    inverse = lax.rsqrt(jnp.mean(target_float * target_float, axis=1, keepdims=True) + EPSILON)
    normed = (target_float * inverse * gain_float).astype(BF)
    tgt_all, src_all, cols = call(
        functools.partial(rows_kernel, sp, tp),
        "rows_kernel",
        1,
        [((2, tp, rows, model), BF), ((tp, srows, model), BF), ((sp, rows, slice_width), BF)],
        [dma((3,)), dma((2, Y)), dma((2, Y)), dma((2, Y)), dma((2, Y)), dma((sp,)), dma((sp,))],
        jnp.stack([normed, output_grad]),
        source_rows,
        normed.reshape(rows, sp, slice_width).transpose(1, 0, 2),
    )
    tgt_all = tgt_all.reshape(2, block, model)
    src_all = src_all.reshape(source_count, model)
    query = jnp.dot(tgt_all[0], query_weight, preferred_element_type=F32).astype(BF)
    head_gradient = contract_last(tgt_all[1], output_weight).astype(BF)
    deltas = jnp.sum(
        (head_gradient.astype(F32) * saved_output.astype(F32)).reshape(block, heads, HEAD_DIM), axis=2
    ).astype(BF)
    small = jnp.pad(jnp.concatenate([norm_offset, deltas], axis=1), ((0, 0), (0, 128 - 2 * heads)))
    q_all, hg_all, small_all, cols_all = call(
        functools.partial(heads_kernel, sp, tp),
        "heads_kernel",
        2,
        [
            ((sp, block, width), BF),
            ((sp, block, width), BF),
            ((sp, block, 128), BF),
            ((sp, tp, rows, slice_width), BF),
        ],
        [dma((4,)), dma((Y,)), dma((Y,)), dma((Y,)), dma((Y,))] + line_sems(Z, 3),
        query,
        head_gradient,
        small,
        cols,
    )
    key = jnp.dot(src_all, key_weight, preferred_element_type=F32).astype(BF)
    value = jnp.dot(src_all, value_weight, preferred_element_type=F32).astype(BF)
    q_heads = q_all.reshape(count, heads, HEAD_DIM)
    hg_heads = hg_all.reshape(count, heads, HEAD_DIM)
    k_heads = key.reshape(source_count, heads, HEAD_DIM)
    v_heads = value.reshape(source_count, heads, HEAD_DIM)
    small_rows = small_all.reshape(count, 128).astype(F32)
    offsets = small_rows[:, :heads].T[:, :, None]
    delta_all = small_rows[:, heads : 2 * heads].T[:, :, None]
    scores = jnp.einsum("rfo,kfo->frk", q_heads, k_heads, preferred_element_type=F32)
    prob = jnp.exp(scores * scale - (shift_base + offsets))
    prob_grad = jnp.einsum("rfo,kfo->frk", hg_heads, v_heads, preferred_element_type=F32)
    score_grad = (prob * (prob_grad - delta_all) * scale).astype(BF)
    prob = prob.astype(BF)
    key_flat = (
        jnp.einsum("wcu,cwp->uwp", score_grad, q_heads, preferred_element_type=F32)
        .astype(BF)
        .reshape(source_count, width)
    )
    value_flat = (
        jnp.einsum("wcu,cwp->uwp", prob, hg_heads, preferred_element_type=F32)
        .astype(BF)
        .reshape(source_count, width)
    )
    query_term = jnp.einsum("tje,etq->jtq", score_grad, k_heads, preferred_element_type=F32)
    query_term = query_term.astype(BF).reshape(sp, block, width)
    source_part = (contract_last(key_flat, key_weight) + contract_last(value_flat, value_weight)).astype(BF)
    vm = pltpu.VMEM
    flat_all, source_grad, normed_grad = call(
        functools.partial(grads_kernel, sp, tp),
        "grads_kernel",
        3,
        [((sp, block, width), BF), ((srows, model), F32), ((rows, model), F32)],
        [vm((Z, block, width), BF)] * 3
        + [vm((Y, srows, model), BF)] * 3
        + [vm((tp, rows, model), BF)]
        + [vm((Y, rows, model), BF)] * 3
        + [dma((Z,))] * 4
        + [dma((Y,))] * 8
        + line_sems(Z, 1),
        query_term,
        source_part.reshape(tp, srows, model),
        query_weight,
    )
    scaled = normed_grad * gain_float
    target_grad = inverse * scaled - target_float * inverse**3 * jnp.mean(
        scaled * target_float, axis=1, keepdims=True
    )
    weight_grad = lax.dot_general(
        cols_all.reshape(count, slice_width),
        flat_all.reshape(count, width),
        (((0,), (0,)), ((), ())),
        preferred_element_type=F32,
    )
    return (target_grad, source_grad, weight_grad)


def solution(mesh):
    in_specs = (
        P(("sp", "tp"), None),
        P(("sp", "tp"), None),
        P(),
        P(None, "tp"),
        P(None, "tp"),
        P(None, "tp"),
        P("tp", None),
        P("sp", "tp"),
        P("sp", "tp"),
        P(("sp", "tp"), None),
    )
    out_specs = (P(("sp", "tp"), None), P(("sp", "tp"), None), P("sp", "tp"))
    return jax.shard_map(body, mesh=mesh, in_specs=in_specs, out_specs=out_specs, check_vma=False)
```

```python
import functools
import math

import jax
import jax.numpy as jnp
from jax import lax
from jax.experimental import pallas as pl
from jax.experimental.pallas import tpu as pltpu
from jax.sharding import PartitionSpec as P

HEAD_DIM = 256
EPSILON = 1e-06
MESH = pl.DeviceIdType.MESH
BF = jnp.bfloat16
F32 = jnp.float32
VMEM = pl.BlockSpec(memory_space=pltpu.VMEM)


def contract_last(left, right):
    return lax.dot_general(left, right, (((1,), (1,)), ((), ())), preferred_element_type=F32)


def push(src, dst, send, recv, device):
    return pltpu.make_async_remote_copy(
        src_ref=src, dst_ref=dst, send_sem=send, recv_sem=recv, device_id=device, device_id_type=MESH
    )


def greet(devices):
    barrier = pltpu.get_barrier_semaphore()
    for device in devices:
        pl.semaphore_signal(barrier, inc=1, device_id=device, device_id_type=MESH)
    pl.semaphore_wait(barrier, len(devices))


class Place:
    def __init__(self, sp, tp):
        self.sp, self.tp, self.Z, self.Y = sp, tp, sp // 2, tp // 2
        self.s, self.t = lax.axis_index("sp"), lax.axis_index("tp")
        self.z, self.x = self.s // 2, self.s % 2
        self.y, self.c = self.t // 2, self.t % 2
        self.partner = (self.s, self.y * 2 + 1 - self.c)
        self.across = (self.z * 2 + 1 - self.x, self.t)

    def chip_y(self, d):
        return (self.s, lax.rem(self.y + d + self.Y, self.Y) * 2 + self.c)

    def chip_z(self, d):
        return (lax.rem(self.z + d + self.Z, self.Z) * 2 + self.x, self.t)


class LineGather:
    def __init__(self, place, pairs, up_s, up_r, dn_s, dn_r, x_s, x_r):
        self.p, self.pairs = place, pairs
        self.sems = (up_s, up_r, dn_s, dn_r, x_s, x_r)

    def up(self, n, d, own=False):
        p, (own_ref, all_ref) = self.p, self.pairs[n]
        block = p.s - 2 * (d - 1)
        src = own_ref if own else all_ref.at[block]
        return push(src, all_ref.at[block], self.sems[0].at[n, d], self.sems[1].at[n, d], (p.s + 2, p.t))

    def up_wait(self, n, d):
        p, (_, all_ref) = self.p, self.pairs[n]
        ref = all_ref.at[p.s - 2 * d]
        return push(ref, ref, self.sems[0].at[n, d], self.sems[1].at[n, d], (p.s - 2, p.t))

    def dn(self, n, d, own=False):
        p, (own_ref, all_ref) = self.p, self.pairs[n]
        block = p.s + 2 * (d - 1)
        src = own_ref if own else all_ref.at[block]
        return push(src, all_ref.at[block], self.sems[2].at[n, d], self.sems[3].at[n, d], (p.s - 2, p.t))

    def dn_wait(self, n, d):
        p, (_, all_ref) = self.p, self.pairs[n]
        ref = all_ref.at[p.s + 2 * d]
        return push(ref, ref, self.sems[2].at[n, d], self.sems[3].at[n, d], (p.s + 2, p.t))

    def over(self, n, d):
        p, (own_ref, all_ref) = self.p, self.pairs[n]
        block = p.s - 2 * d
        k = d + p.Z - 1
        src = own_ref if d == 0 else all_ref.at[block]
        return push(src, all_ref.at[block], self.sems[4].at[n, k], self.sems[5].at[n, k], p.across)

    def over_wait(self, n, d):
        p, (_, all_ref) = self.p, self.pairs[n]
        ref = all_ref.at[p.z * 2 + 1 - p.x - 2 * d]
        k = d + p.Z - 1
        return push(ref, ref, self.sems[4].at[n, k], self.sems[5].at[n, k], p.across)

    def start(self, count):
        p = self.p

        @pl.when(p.z + 1 < p.Z)
        def _():
            for n in count:
                self.up(n, 1, True).start()

        @pl.when(p.z >= 1)
        def _():
            for n in count:
                self.dn(n, 1, True).start()

        for n in count:
            self.over(n, 0).start()

    def step(self, d):
        p = self.p
        for n in range(len(self.pairs)):

            @pl.when(p.z - d >= 0)
            def _():
                self.up_wait(n, d).wait_recv()

                @pl.when(p.z + 1 < p.Z)
                def _():
                    self.up(n, d + 1).start()

                self.over(n, d).start()

            @pl.when(p.z + d < p.Z)
            def _():
                self.dn_wait(n, d).wait_recv()

                @pl.when(p.z >= 1)
                def _():
                    self.dn(n, d + 1).start()

                self.over(n, -d).start()

    def arrive(self, sign, d):
        for n in range(len(self.pairs)):
            self.over_wait(n, sign * d).wait_recv()

    def side(self, sign, d):
        return self.p.z - d >= 0 if sign > 0 else self.p.z + d < self.p.Z

    def finish(self):
        p = self.p
        for n in range(len(self.pairs)):
            for d in range(p.Z):
                for sign in (1, -1) if d else (1,):

                    @pl.when(self.side(sign, d))
                    def _():
                        self.over(n, sign * d).wait_send()

            for d in range(1, p.Z):

                @pl.when(jnp.logical_and(p.z - d + 1 >= 0, p.z + 1 < p.Z))
                def _():
                    self.up(n, d).wait_send()

                @pl.when(jnp.logical_and(p.z + d - 1 < p.Z, p.z >= 1))
                def _():
                    self.dn(n, d).wait_send()


def line_sems(p_z, n):
    return [pltpu.SemaphoreType.DMA((n, p_z + 1))] * 4 + [pltpu.SemaphoreType.DMA((n, 2 * p_z))] * 2


class PairScatter:
    def __init__(self, p, part, first, summed, second, fs, fr, ss, sr):
        self.p, self.part, self.first, self.summed, self.second = p, part, first, summed, second
        self.sems = (fs, fr, ss, sr)
        self.started = []

    def start(self):
        p = self.p
        for d in range(p.Y):
            y = lax.rem(p.y + d, p.Y)
            copy = push(
                self.part(y * 2 + 1 - p.c), self.first.at[d], self.sems[0].at[d], self.sems[1].at[d], p.partner
            )
            copy.start()
            self.started.append(copy)

    def middle(self):
        p = self.p
        for d in list(range(1, p.Y)) + [0]:
            y = lax.rem(p.y + d, p.Y)
            self.started[d].wait_recv()
            total = self.part(y * 2 + p.c)[...].astype(F32) + self.first[d].astype(F32)
            self.summed[d] = total.astype(BF)
            if d:
                copy = push(
                    self.summed.at[d], self.second.at[d], self.sems[2].at[d], self.sems[3].at[d], p.chip_y(d)
                )
                copy.start()
                self.started.append(copy)

    def finish(self):
        p = self.p
        total = self.part(p.t)[...].astype(F32) + self.first[0].astype(F32)
        for d in range(1, p.Y):
            self.started[p.Y + d - 1].wait_recv()
            total = total + self.second[d].astype(F32)
        for copy in self.started:
            copy.wait_send()
        return total


class PairGather:
    def __init__(self, p, own, spot, ys, yr, ps, pr):
        self.p, self.own, self.spot, self.sems = p, own, spot, (ys, yr, ps, pr)
        self.started = []

    def start(self):
        p = self.p
        for d in range(1, p.Y):
            copy = push(self.own, self.spot(p.t), self.sems[0].at[d], self.sems[1].at[d], p.chip_y(d))
            copy.start()
            self.started.append(copy)
        copy = push(self.own, self.spot(p.t), self.sems[2].at[0], self.sems[3].at[0], p.partner)
        copy.start()
        self.started.append(copy)

    def forward(self):
        p = self.p
        for d in range(1, p.Y):
            ref = self.spot(lax.rem(p.y - d + p.Y, p.Y) * 2 + p.c)
            push(ref, ref, self.sems[0].at[d], self.sems[1].at[d], p.chip_y(-d)).wait_recv()
            copy = push(ref, ref, self.sems[2].at[d], self.sems[3].at[d], p.partner)
            copy.start()
            self.started.append(copy)

    def arrive(self):
        p = self.p
        for d in range(p.Y):
            ref = self.spot(lax.rem(p.y - d + p.Y, p.Y) * 2 + 1 - p.c)
            push(ref, ref, self.sems[2].at[d], self.sems[3].at[d], p.partner).wait_recv()

    def finish(self):
        for copy in self.started:
            copy.wait_send()


def layer_kernel(
    sp, tp, shift_base,
    tn, to, src, pieces, saved, offs, wq_h, wk_h, wv_h, wo_h,
    flat_all, src_out, ng_out, cols_all,
    wq, wk, wv, wo, tn_all, to_all, src_all, cols, tn_b, to_b,
    q_all, hg_all, small_all, k_s, v_s, p_s, d_s, part, kf, vf, sg,
    xr, xz, zr, sg1, sg2, sg3, ng, ng1, ng2, ng3,
    wsem, loc, es, er, *sems
):
    p = Place(sp, tp)
    pair_sems = [sems[4 * i : 4 * i + 4] for i in range(6)]
    xs_s, xs_r, zs_s, zs_r = sems[24:28]
    line_a, line_b = sems[28:34], sems[34:40]
    rows, block = tn.shape[0], saved.shape[0]
    width, model = wq.shape[1], wq.shape[0]
    heads = width // HEAD_DIM
    scale = HEAD_DIM ** (-0.5)
    loads = [
        pltpu.make_async_copy(h, v, wsem.at[i])
        for i, (h, v) in enumerate(((wq_h, wq), (wo_h, wo), (wk_h, wk), (wv_h, wv)))
    ]
    for copy in loads:
        copy.start()
    greet(
        [p.partner]
        + [p.chip_y(d) for d in range(1, p.Y)]
        + [(lax.rem(p.s + e, sp), p.t) for e in range(1, sp)]
    )
    g_tn = PairGather(p, tn, lambda t: tn_all.at[t], *pair_sems[0])
    g_to = PairGather(p, to, lambda t: to_all.at[t], *pair_sems[1])
    g_src = PairGather(p, src, lambda t: src_all.at[t], *pair_sems[2])
    g_cols = PairGather(p, cols, lambda t: cols_all.at[:, t], *pair_sems[3])
    for g in (g_tn, g_to, g_src):
        g.start()
    swaps = []
    for e in range(1, sp):
        s = lax.rem(p.s + e, sp)
        copy = push(pieces.at[s], cols.at[p.s], es.at[e], er.at[e], (s, p.t))
        copy.start()
        swaps.append(copy)
    mine = [
        pltpu.make_async_copy(tn, tn_all.at[p.t], loc.at[0]),
        pltpu.make_async_copy(to, to_all.at[p.t], loc.at[1]),
        pltpu.make_async_copy(src, src_all.at[p.t], loc.at[2]),
        pltpu.make_async_copy(pieces.at[p.s], cols.at[p.s], loc.at[3]),
    ]
    for copy in mine:
        copy.start()
    for copy in mine:
        copy.wait()
    tile = min(width, 256)
    gather = LineGather(
        p, ((q_all.at[p.s], q_all), (hg_all.at[p.s], hg_all), (small_all.at[p.s], small_all)), *line_a
    )

    g_tn.forward()
    g_to.forward()
    g_tn.arrive()
    for t in range(tp):
        tn_b[t * rows : (t + 1) * rows, :] = tn_all[t]
    loads[0].wait()
    for j in range(0, width, tile):
        q_all[p.s, :, j : j + tile] = jnp.dot(
            tn_b[...], wq[:, j : j + tile], preferred_element_type=F32
        ).astype(BF)
    gather.start((0,))
    g_to.arrive()
    for t in range(tp):
        to_b[t * rows : (t + 1) * rows, :] = to_all[t]
    loads[1].wait()
    lane = lax.broadcasted_iota(jnp.int32, (block, 128), 1)
    small = jnp.zeros((block, 128), F32)
    off_value = offs[...].astype(F32)
    for h in range(heads):
        cut = slice(h * HEAD_DIM, (h + 1) * HEAD_DIM)
        part_h = contract_last(to_b[...], wo[cut, :]).astype(BF)
        hg_all[p.s, :, cut] = part_h
        delta = jnp.sum(part_h.astype(F32) * saved[:, cut].astype(F32), axis=1, keepdims=True)
        small = jnp.where(lane == h, off_value[:, h : h + 1], small)
        small = jnp.where(lane == heads + h, delta, small)
    small_all[p.s] = small.astype(BF)
    gather.start((1, 2))

    g_src.forward()
    g_src.arrive()
    source_count = k_s.shape[0]
    loads[2].wait()
    loads[3].wait()

    @pl.loop(0, width // tile)
    def _(j):
        cut = pl.ds(pl.multiple_of(j * tile, tile), tile)
        rows_value = src_all[...].reshape(source_count, model)
        k_s[:, cut] = jnp.dot(rows_value, wk[:, cut], preferred_element_type=F32).astype(BF)
        v_s[:, cut] = jnp.dot(rows_value, wv[:, cut], preferred_element_type=F32).astype(BF)

    for e in range(1, sp):
        s = lax.rem(p.s - e + sp, sp)
        push(cols.at[s], cols.at[s], es.at[e], er.at[e], (s, p.t)).wait_recv()
    g_cols.start()
    keep = pltpu.make_async_copy(cols, cols_all.at[:, p.t], loc.at[4])
    keep.start()

    def into(k):
        z = lax.rem(p.z + k, p.Z)
        return push(part.at[z * 2 + 1 - p.x], xr.at[k], xs_s.at[k], xs_r.at[k], p.across)

    def attend(z):
        pair = pl.ds(2 * z, 2)
        spot = pl.ds(pl.multiple_of(z * (2 * block), 2 * block), 2 * block)
        tiny = small_all[pair].reshape(2 * block, 128).astype(F32)
        for h in range(heads):
            cut = slice(h * HEAD_DIM, (h + 1) * HEAD_DIM)
            q_h = q_all[pair, :, cut].reshape(2 * block, HEAD_DIM)
            g_h = hg_all[pair, :, cut].reshape(2 * block, HEAD_DIM)
            prob = jnp.exp(contract_last(q_h, k_s[:, cut]) * scale - (shift_base + tiny[:, h : h + 1]))
            grad = contract_last(g_h, v_s[:, cut])
            score = (prob * (grad - tiny[:, heads + h : heads + h + 1]) * scale).astype(BF)
            p_s[h, spot, :] = prob.astype(BF)
            d_s[h, spot, :] = score
            term = jnp.dot(score, k_s[:, cut], preferred_element_type=F32).astype(BF)
            part[pair, :, cut] = term.reshape(2, block, HEAD_DIM)

    def reached(sign, d):
        gather.arrive(sign, d)
        attend(p.z - sign * d)
        into((-sign * d) % p.Z).start()

    for d in range(1, p.Z):
        gather.step(d)
        for sign in (1, -1) if d > 1 else (1,):

            @pl.when(gather.side(sign, d - 1))
            def _():
                reached(sign, d - 1)

        if d == 1:
            g_cols.forward()
    for sign in (1, -1):

        @pl.when(gather.side(sign, p.Z - 1))
        def _():
            reached(sign, p.Z - 1)

    order = sorted(range(1, p.Z), key=lambda k: min(k, p.Z - k))
    hops = {}

    def relay(k):
        into(k).wait_recv()
        z = lax.rem(p.z + k, p.Z)
        xz[k] = (part[z * 2 + p.x].astype(F32) + xr[k].astype(F32)).astype(BF)
        hops[k] = push(xz.at[k], zr.at[k], zs_s.at[k], zs_r.at[k], p.chip_z(k))
        hops[k].start()

    for k in order[:1]:
        relay(k)
    count = sp * block

    for h in range(heads):
        cut = slice(h * HEAD_DIM, (h + 1) * HEAD_DIM)
        dims = (((0,), (0,)), ((), ()))
        q_h = q_all[:, :, cut].reshape(count, HEAD_DIM)
        g_h = hg_all[:, :, cut].reshape(count, HEAD_DIM)
        kf[:, cut] = lax.dot_general(d_s[h], q_h, dims, preferred_element_type=F32).astype(BF)
        vf[:, cut] = lax.dot_general(p_s[h], g_h, dims, preferred_element_type=F32).astype(BF)
    for k in order[1:2]:
        relay(k)
    stile = min(model, 256)

    @pl.loop(0, model // stile)
    def _(j):
        cut = pl.ds(pl.multiple_of(j * stile, stile), stile)
        value = contract_last(kf[...], wk[cut, :]) + contract_last(vf[...], wv[cut, :])
        sg[:, :, cut] = value.astype(BF).reshape(tp, source_count // tp, stile)

    source = PairScatter(p, lambda t: sg.at[t], sg1, sg2, sg3, *pair_sems[4])
    source.start()
    for k in order[2:]:
        relay(k)
    source.middle()
    into(0).wait_recv()
    total = part[p.s].astype(F32) + xr[0].astype(F32)
    for k in order:
        hops[k].wait_recv()
        total = total + zr[k].astype(F32)
    flat = total.astype(BF)
    flat_all[p.s] = flat
    spread = LineGather(p, ((flat_all.at[p.s], flat_all),), *line_b)
    spread.start((0,))
    for j in range(0, model, stile):
        columns = contract_last(flat, wq[j : j + stile, :]).astype(BF)
        for t in range(tp):
            ng[t, :, j : j + stile] = columns[t * rows : (t + 1) * rows]
    normed = PairScatter(p, lambda t: ng.at[t], ng1, ng2, ng3, *pair_sems[5])
    normed.start()
    for d in range(1, p.Z):
        spread.step(d)
        if d == 1:
            normed.middle()
    src_out[...] = source.finish()
    ng_out[...] = normed.finish()
    g_cols.arrive()
    for d in range(p.Z):
        for sign in (1, -1) if d else (1,):

            @pl.when(spread.side(sign, d))
            def _():
                spread.arrive(sign, d)

    gather.finish()
    spread.finish()
    for g in (g_tn, g_to, g_src, g_cols):
        g.finish()
    for copy in swaps:
        copy.wait_send()
    keep.wait()
    for k in range(p.Z):
        into(k).wait_send()
    for k in order:
        hops[k].wait_send()


def body(
    target_rows,
    source_rows,
    norm_gain,
    query_weight,
    key_weight,
    value_weight,
    output_weight,
    saved_output,
    norm_offset,
    output_grad,
):
    tp, sp = lax.axis_size("tp"), lax.axis_size("sp")
    Z, Y = sp // 2, tp // 2
    model, width = query_weight.shape
    heads = width // HEAD_DIM
    rows, srows = target_rows.shape[0], source_rows.shape[0]
    block = rows * tp
    count = block * sp
    source_count = srows * tp
    shift_base = math.log(source_count * sp)
    slice_width = model // sp
    dma = pltpu.SemaphoreType.DMA

    target_float = target_rows.astype(F32)
    gain_float = norm_gain.astype(F32)
    inverse = lax.rsqrt(jnp.mean(target_float * target_float, axis=1, keepdims=True) + EPSILON)
    normed = (target_float * inverse * gain_float).astype(BF)
    vm = pltpu.VMEM
    whole = pl.BlockSpec(memory_space=pl.ANY)
    flat_all, source_grad, normed_grad, cols_all = pl.pallas_call(
        functools.partial(layer_kernel, sp, tp, shift_base),
        out_shape=[
            jax.ShapeDtypeStruct((sp, block, width), BF),
            jax.ShapeDtypeStruct((srows, model), F32),
            jax.ShapeDtypeStruct((rows, model), F32),
            jax.ShapeDtypeStruct((sp, tp, rows, slice_width), BF),
        ],
        in_specs=[VMEM] * 6 + [whole] * 4,
        out_specs=[VMEM] * 4,
        scratch_shapes=[vm((model, width), BF)] * 3
        + [vm((width, model), BF)]
        + [vm((tp, rows, model), BF)] * 2
        + [vm((tp, srows, model), BF), vm((sp, rows, slice_width), BF)]
        + [vm((block, model), BF)] * 2
        + [vm((sp, block, width), BF)] * 2
        + [vm((sp, block, 128), BF)]
        + [vm((source_count, width), BF)] * 2
        + [vm((heads, count, source_count), BF)] * 2
        + [vm((sp, block, width), BF)]
        + [vm((source_count, width), BF)] * 2
        + [vm((tp, srows, model), BF)]
        + [vm((Z, block, width), BF)] * 3
        + [vm((Y, srows, model), BF)] * 3
        + [vm((tp, rows, model), BF)]
        + [vm((Y, rows, model), BF)] * 3
        + [dma((4,)), dma((5,)), dma((sp,)), dma((sp,))]
        + [dma((Y,))] * 24
        + [dma((Z,))] * 4
        + line_sems(Z, 3)
        + line_sems(Z, 1),
        name="layer_kernel",
        compiler_params=pltpu.CompilerParams(
            collective_id=1, has_side_effects=True, vmem_limit_bytes=58 * 2**20
        ),
    )(
        normed,
        output_grad,
        source_rows,
        normed.reshape(rows, sp, slice_width).transpose(1, 0, 2),
        saved_output,
        norm_offset,
        query_weight,
        key_weight,
        value_weight,
        output_weight,
    )
    scaled = normed_grad * gain_float
    target_grad = inverse * scaled - target_float * inverse**3 * jnp.mean(
        scaled * target_float, axis=1, keepdims=True
    )
    weight_grad = lax.dot_general(
        cols_all.reshape(count, slice_width),
        flat_all.reshape(count, width),
        (((0,), (0,)), ((), ())),
        preferred_element_type=F32,
    )
    return (target_grad, source_grad, weight_grad)


def solution(mesh):
    in_specs = (
        P(("sp", "tp"), None),
        P(("sp", "tp"), None),
        P(),
        P(None, "tp"),
        P(None, "tp"),
        P(None, "tp"),
        P("tp", None),
        P("sp", "tp"),
        P("sp", "tp"),
        P(("sp", "tp"), None),
    )
    out_specs = (P(("sp", "tp"), None), P(("sp", "tp"), None), P("sp", "tp"))
    return jax.shard_map(body, mesh=mesh, in_specs=in_specs, out_specs=out_specs, check_vma=False)
```

```python
import functools
import math

import jax
import jax.numpy as jnp
from jax import lax
from jax.experimental import pallas as pl
from jax.experimental.pallas import tpu as pltpu
from jax.sharding import PartitionSpec as P

HEAD_DIM = 256
EPSILON = 1e-06
MESH = pl.DeviceIdType.MESH
BF = jnp.bfloat16
F32 = jnp.float32
VMEM = pl.BlockSpec(memory_space=pltpu.VMEM)


def contract_last(left, right):
    return lax.dot_general(left, right, (((1,), (1,)), ((), ())), preferred_element_type=F32)


def push(src, dst, send, recv, device):
    return pltpu.make_async_remote_copy(
        src_ref=src, dst_ref=dst, send_sem=send, recv_sem=recv, device_id=device, device_id_type=MESH
    )


def greet(devices):
    barrier = pltpu.get_barrier_semaphore()
    for device in devices:
        pl.semaphore_signal(barrier, inc=1, device_id=device, device_id_type=MESH)
    pl.semaphore_wait(barrier, len(devices))


class Place:
    def __init__(self, sp, tp):
        self.sp, self.tp, self.Z, self.Y = sp, tp, sp // 2, tp // 2
        self.s, self.t = lax.axis_index("sp"), lax.axis_index("tp")
        self.z, self.x = self.s // 2, self.s % 2
        self.y, self.c = self.t // 2, self.t % 2
        self.partner = (self.s, self.y * 2 + 1 - self.c)
        self.across = (self.z * 2 + 1 - self.x, self.t)

    def chip_y(self, d):
        return (self.s, lax.rem(self.y + d + self.Y, self.Y) * 2 + self.c)

    def chip_z(self, d):
        return (lax.rem(self.z + d + self.Z, self.Z) * 2 + self.x, self.t)


class LineGather:
    def __init__(self, place, pairs, up_s, up_r, dn_s, dn_r, x_s, x_r):
        self.p, self.pairs = place, pairs
        self.sems = (up_s, up_r, dn_s, dn_r, x_s, x_r)

    def up(self, n, d, own=False):
        p, (own_ref, all_ref) = self.p, self.pairs[n]
        block = p.s - 2 * (d - 1)
        src = own_ref if own else all_ref.at[block]
        return push(src, all_ref.at[block], self.sems[0].at[n, d], self.sems[1].at[n, d], (p.s + 2, p.t))

    def up_wait(self, n, d):
        p, (_, all_ref) = self.p, self.pairs[n]
        ref = all_ref.at[p.s - 2 * d]
        return push(ref, ref, self.sems[0].at[n, d], self.sems[1].at[n, d], (p.s - 2, p.t))

    def dn(self, n, d, own=False):
        p, (own_ref, all_ref) = self.p, self.pairs[n]
        block = p.s + 2 * (d - 1)
        src = own_ref if own else all_ref.at[block]
        return push(src, all_ref.at[block], self.sems[2].at[n, d], self.sems[3].at[n, d], (p.s - 2, p.t))

    def dn_wait(self, n, d):
        p, (_, all_ref) = self.p, self.pairs[n]
        ref = all_ref.at[p.s + 2 * d]
        return push(ref, ref, self.sems[2].at[n, d], self.sems[3].at[n, d], (p.s + 2, p.t))

    def over(self, n, d):
        p, (own_ref, all_ref) = self.p, self.pairs[n]
        block = p.s - 2 * d
        k = d + p.Z - 1
        src = own_ref if d == 0 else all_ref.at[block]
        return push(src, all_ref.at[block], self.sems[4].at[n, k], self.sems[5].at[n, k], p.across)

    def over_wait(self, n, d):
        p, (_, all_ref) = self.p, self.pairs[n]
        ref = all_ref.at[p.z * 2 + 1 - p.x - 2 * d]
        k = d + p.Z - 1
        return push(ref, ref, self.sems[4].at[n, k], self.sems[5].at[n, k], p.across)

    def start(self, count):
        p = self.p

        @pl.when(p.z + 1 < p.Z)
        def _():
            for n in count:
                self.up(n, 1, True).start()

        @pl.when(p.z >= 1)
        def _():
            for n in count:
                self.dn(n, 1, True).start()

        for n in count:
            self.over(n, 0).start()

    def step(self, d):
        p = self.p
        for n in range(len(self.pairs)):

            @pl.when(p.z - d >= 0)
            def _():
                self.up_wait(n, d).wait_recv()

                @pl.when(p.z + 1 < p.Z)
                def _():
                    self.up(n, d + 1).start()

                self.over(n, d).start()

            @pl.when(p.z + d < p.Z)
            def _():
                self.dn_wait(n, d).wait_recv()

                @pl.when(p.z >= 1)
                def _():
                    self.dn(n, d + 1).start()

                self.over(n, -d).start()

    def arrive(self, sign, d):
        for n in range(len(self.pairs)):
            self.over_wait(n, sign * d).wait_recv()

    def side(self, sign, d):
        return self.p.z - d >= 0 if sign > 0 else self.p.z + d < self.p.Z

    def finish(self):
        p = self.p
        for n in range(len(self.pairs)):
            for d in range(p.Z):
                for sign in (1, -1) if d else (1,):

                    @pl.when(self.side(sign, d))
                    def _():
                        self.over(n, sign * d).wait_send()

            for d in range(1, p.Z):

                @pl.when(jnp.logical_and(p.z - d + 1 >= 0, p.z + 1 < p.Z))
                def _():
                    self.up(n, d).wait_send()

                @pl.when(jnp.logical_and(p.z + d - 1 < p.Z, p.z >= 1))
                def _():
                    self.dn(n, d).wait_send()


def line_sems(p_z, n):
    return [pltpu.SemaphoreType.DMA((n, p_z + 1))] * 4 + [pltpu.SemaphoreType.DMA((n, 2 * p_z))] * 2


class PairScatter:
    def __init__(self, p, part, first, summed, second, fs, fr, ss, sr):
        self.p, self.part, self.first, self.summed, self.second = p, part, first, summed, second
        self.sems = (fs, fr, ss, sr)
        self.started = []

    def start(self):
        p = self.p
        for d in range(p.Y):
            y = lax.rem(p.y + d, p.Y)
            copy = push(
                self.part(y * 2 + 1 - p.c), self.first.at[d], self.sems[0].at[d], self.sems[1].at[d], p.partner
            )
            copy.start()
            self.started.append(copy)

    def middle(self):
        p = self.p
        for d in list(range(1, p.Y)) + [0]:
            y = lax.rem(p.y + d, p.Y)
            self.started[d].wait_recv()
            total = self.part(y * 2 + p.c)[...].astype(F32) + self.first[d].astype(F32)
            self.summed[d] = total.astype(BF)
            if d:
                copy = push(
                    self.summed.at[d], self.second.at[d], self.sems[2].at[d], self.sems[3].at[d], p.chip_y(d)
                )
                copy.start()
                self.started.append(copy)

    def finish(self):
        p = self.p
        total = self.part(p.t)[...].astype(F32) + self.first[0].astype(F32)
        for d in range(1, p.Y):
            self.started[p.Y + d - 1].wait_recv()
            total = total + self.second[d].astype(F32)
        for copy in self.started:
            copy.wait_send()
        return total


class PairGather:
    def __init__(self, p, own, spot, ys, yr, ps, pr):
        self.p, self.own, self.spot, self.sems = p, own, spot, (ys, yr, ps, pr)
        self.started = []

    def start(self):
        p = self.p
        for d in range(1, p.Y):
            copy = push(self.own, self.spot(p.t), self.sems[0].at[d], self.sems[1].at[d], p.chip_y(d))
            copy.start()
            self.started.append(copy)
        copy = push(self.own, self.spot(p.t), self.sems[2].at[0], self.sems[3].at[0], p.partner)
        copy.start()
        self.started.append(copy)

    def forward(self):
        p = self.p
        for d in range(1, p.Y):
            ref = self.spot(lax.rem(p.y - d + p.Y, p.Y) * 2 + p.c)
            push(ref, ref, self.sems[0].at[d], self.sems[1].at[d], p.chip_y(-d)).wait_recv()
            copy = push(ref, ref, self.sems[2].at[d], self.sems[3].at[d], p.partner)
            copy.start()
            self.started.append(copy)

    def arrive(self):
        p = self.p
        for d in range(p.Y):
            ref = self.spot(lax.rem(p.y - d + p.Y, p.Y) * 2 + 1 - p.c)
            push(ref, ref, self.sems[2].at[d], self.sems[3].at[d], p.partner).wait_recv()

    def finish(self):
        for copy in self.started:
            copy.wait_send()


def layer_kernel(
    sp, tp, shift_base,
    raw, to, src, gain, saved, offs, wq_h, wk_h, wv_h, wo_h,
    flat_all, src_out, tgt_out, cols_all,
    tn, pieces, wq, wk, wv, wo, tn_all, to_all, src_all, cols, tn_b, to_b,
    q_all, hg_all, small_all, k_s, v_s, p_s, d_s, part, kf, vf, sg,
    xr, xz, zr, sg1, sg2, sg3, ng, ng1, ng2, ng3,
    wsem, loc, es, er, *sems
):
    p = Place(sp, tp)
    pair_sems = [sems[4 * i : 4 * i + 4] for i in range(6)]
    xs_s, xs_r, zs_s, zs_r = sems[24:28]
    line_a, line_b = sems[28:34], sems[34:40]
    rows, block = raw.shape[0], saved.shape[0]
    width, model = wq.shape[1], wq.shape[0]
    heads = width // HEAD_DIM
    scale = HEAD_DIM ** (-0.5)
    loads = [
        pltpu.make_async_copy(h, v, wsem.at[i])
        for i, (h, v) in enumerate(((wq_h, wq), (wo_h, wo), (wk_h, wk), (wv_h, wv)))
    ]
    for copy in loads:
        copy.start()
    raw_value, gain_value = raw[...].astype(F32), gain[...].astype(F32)
    inverse = lax.rsqrt(jnp.mean(raw_value * raw_value, axis=1, keepdims=True) + EPSILON)
    normed_value = (raw_value * inverse * gain_value).astype(BF)
    tn[...] = normed_value
    slice_width = model // sp
    for s in range(sp):
        pieces[s] = normed_value[:, s * slice_width : (s + 1) * slice_width]
    greet(
        [p.partner]
        + [p.chip_y(d) for d in range(1, p.Y)]
        + [(lax.rem(p.s + e, sp), p.t) for e in range(1, sp)]
    )
    g_tn = PairGather(p, tn, lambda t: tn_all.at[t], *pair_sems[0])
    g_to = PairGather(p, to, lambda t: to_all.at[t], *pair_sems[1])
    g_src = PairGather(p, src, lambda t: src_all.at[t], *pair_sems[2])
    g_cols = PairGather(p, cols, lambda t: cols_all.at[:, t], *pair_sems[3])
    for g in (g_tn, g_to, g_src):
        g.start()
    swaps = []
    for e in range(1, sp):
        s = lax.rem(p.s + e, sp)
        copy = push(pieces.at[s], cols.at[p.s], es.at[e], er.at[e], (s, p.t))
        copy.start()
        swaps.append(copy)
    mine = [
        pltpu.make_async_copy(tn, tn_all.at[p.t], loc.at[0]),
        pltpu.make_async_copy(to, to_all.at[p.t], loc.at[1]),
        pltpu.make_async_copy(src, src_all.at[p.t], loc.at[2]),
        pltpu.make_async_copy(pieces.at[p.s], cols.at[p.s], loc.at[3]),
    ]
    for copy in mine:
        copy.start()
    for copy in mine:
        copy.wait()
    tile = min(width, 256)
    gather = LineGather(
        p, ((q_all.at[p.s], q_all), (hg_all.at[p.s], hg_all), (small_all.at[p.s], small_all)), *line_a
    )

    g_tn.forward()
    g_to.forward()
    g_tn.arrive()
    for t in range(tp):
        tn_b[t * rows : (t + 1) * rows, :] = tn_all[t]
    loads[0].wait()
    for j in range(0, width, tile):
        q_all[p.s, :, j : j + tile] = jnp.dot(
            tn_b[...], wq[:, j : j + tile], preferred_element_type=F32
        ).astype(BF)
    gather.start((0,))
    g_to.arrive()
    for t in range(tp):
        to_b[t * rows : (t + 1) * rows, :] = to_all[t]
    loads[1].wait()
    lane = lax.broadcasted_iota(jnp.int32, (block, 128), 1)
    pick = lax.broadcasted_iota(jnp.int32, (heads, 128), 0) == lax.broadcasted_iota(jnp.int32, (heads, 128), 1)
    small = lax.dot_general(
        offs[...].astype(F32), pick.astype(F32), (((0,), (0,)), ((), ())), precision=lax.Precision.HIGHEST,
        preferred_element_type=F32,
    )
    for h in range(heads):
        cut = slice(h * HEAD_DIM, (h + 1) * HEAD_DIM)
        part_h = contract_last(to_b[...], wo[cut, :]).astype(BF)
        hg_all[p.s, :, cut] = part_h
        delta = jnp.sum(part_h.astype(F32) * saved[:, cut].astype(F32), axis=1, keepdims=True)
        small = jnp.where(lane == heads + h, delta, small)
    small_all[p.s] = small.astype(BF)
    gather.start((1, 2))

    g_src.forward()
    g_src.arrive()
    gather.step(1)
    source_count = k_s.shape[0]
    loads[2].wait()
    loads[3].wait()

    @pl.loop(0, width // tile)
    def _(j):
        cut = pl.ds(pl.multiple_of(j * tile, tile), tile)
        rows_value = src_all[...].reshape(source_count, model)
        k_s[:, cut] = jnp.dot(rows_value, wk[:, cut], preferred_element_type=F32).astype(BF)
        v_s[:, cut] = jnp.dot(rows_value, wv[:, cut], preferred_element_type=F32).astype(BF)

    for e in range(1, sp):
        s = lax.rem(p.s - e + sp, sp)
        push(cols.at[s], cols.at[s], es.at[e], er.at[e], (s, p.t)).wait_recv()
    g_cols.start()
    keep = pltpu.make_async_copy(cols, cols_all.at[:, p.t], loc.at[4])
    keep.start()

    def into(k):
        z = lax.rem(p.z + k, p.Z)
        return push(part.at[z * 2 + 1 - p.x], xr.at[k], xs_s.at[k], xs_r.at[k], p.across)

    def attend(z):
        pair = pl.ds(2 * z, 2)
        spot = pl.ds(pl.multiple_of(z * (2 * block), 2 * block), 2 * block)
        tiny = small_all[pair].reshape(2 * block, 128).astype(F32)
        for h in range(heads):
            cut = slice(h * HEAD_DIM, (h + 1) * HEAD_DIM)
            q_h = q_all[pair, :, cut].reshape(2 * block, HEAD_DIM)
            g_h = hg_all[pair, :, cut].reshape(2 * block, HEAD_DIM)
            prob = jnp.exp(contract_last(q_h, k_s[:, cut]) * scale - (shift_base + tiny[:, h : h + 1]))
            grad = contract_last(g_h, v_s[:, cut])
            score = (prob * (grad - tiny[:, heads + h : heads + h + 1]) * scale).astype(BF)
            p_s[h, spot, :] = prob.astype(BF)
            d_s[h, spot, :] = score
            term = jnp.dot(score, k_s[:, cut], preferred_element_type=F32).astype(BF)
            part[pair, :, cut] = term.reshape(2, block, HEAD_DIM)

    def reached(sign, d):
        gather.arrive(sign, d)
        attend(p.z - sign * d)
        into((-sign * d) % p.Z).start()

    for d in range(1, p.Z):
        if d > 1:
            gather.step(d)
        for sign in (1, -1) if d > 1 else (1,):

            @pl.when(gather.side(sign, d - 1))
            def _():
                reached(sign, d - 1)

        if d == 1:
            g_cols.forward()
    for sign in (1, -1):

        @pl.when(gather.side(sign, p.Z - 1))
        def _():
            reached(sign, p.Z - 1)

    order = sorted(range(1, p.Z), key=lambda k: min(k, p.Z - k))
    hops = {}

    def relay(k):
        into(k).wait_recv()
        z = lax.rem(p.z + k, p.Z)
        xz[k] = (part[z * 2 + p.x].astype(F32) + xr[k].astype(F32)).astype(BF)
        hops[k] = push(xz.at[k], zr.at[k], zs_s.at[k], zs_r.at[k], p.chip_z(k))
        hops[k].start()

    for k in order[:1]:
        relay(k)
    count = sp * block

    for h in range(heads):
        cut = slice(h * HEAD_DIM, (h + 1) * HEAD_DIM)
        dims = (((0,), (0,)), ((), ()))
        q_h = q_all[:, :, cut].reshape(count, HEAD_DIM)
        g_h = hg_all[:, :, cut].reshape(count, HEAD_DIM)
        kf[:, cut] = lax.dot_general(d_s[h], q_h, dims, preferred_element_type=F32).astype(BF)
        vf[:, cut] = lax.dot_general(p_s[h], g_h, dims, preferred_element_type=F32).astype(BF)
    for k in order[1:2]:
        relay(k)
    stile = min(model, 256)

    def source_term(j):
        cut = pl.ds(pl.multiple_of(j * stile, stile), stile)
        value = contract_last(kf[...], wk[cut, :]) + contract_last(vf[...], wv[cut, :])
        sg[:, :, cut] = value.astype(BF).reshape(tp, source_count // tp, stile)

    half = model // stile // 2
    pl.loop(0, half)(source_term)
    for k in order[2:]:
        relay(k)
    pl.loop(half, model // stile)(source_term)
    source = PairScatter(p, lambda t: sg.at[t], sg1, sg2, sg3, *pair_sems[4])
    source.start()
    source.middle()
    into(0).wait_recv()
    total = part[p.s].astype(F32) + xr[0].astype(F32)
    for k in order:
        hops[k].wait_recv()
        total = total + zr[k].astype(F32)
    flat = total.astype(BF)
    flat_all[p.s] = flat
    spread = LineGather(p, ((flat_all.at[p.s], flat_all),), *line_b)
    spread.start((0,))
    for j in range(0, model, stile):
        columns = contract_last(flat, wq[j : j + stile, :]).astype(BF)
        for t in range(tp):
            ng[t, :, j : j + stile] = columns[t * rows : (t + 1) * rows]
    normed = PairScatter(p, lambda t: ng.at[t], ng1, ng2, ng3, *pair_sems[5])
    normed.start()
    for d in range(1, p.Z):
        spread.step(d)
        if d == 1:
            normed.middle()
    src_out[...] = source.finish()
    raw_value, gain_value = raw[...].astype(F32), gain[...].astype(F32)
    inverse = lax.rsqrt(jnp.mean(raw_value * raw_value, axis=1, keepdims=True) + EPSILON)
    scaled = normed.finish() * gain_value
    tgt_out[...] = inverse * scaled - raw_value * (inverse * inverse * inverse) * jnp.mean(
        scaled * raw_value, axis=1, keepdims=True
    )
    g_cols.arrive()
    for d in range(p.Z):
        for sign in (1, -1) if d else (1,):

            @pl.when(spread.side(sign, d))
            def _():
                spread.arrive(sign, d)

    gather.finish()
    spread.finish()
    for g in (g_tn, g_to, g_src, g_cols):
        g.finish()
    for copy in swaps:
        copy.wait_send()
    keep.wait()
    for k in range(p.Z):
        into(k).wait_send()
    for k in order:
        hops[k].wait_send()


def body(
    target_rows,
    source_rows,
    norm_gain,
    query_weight,
    key_weight,
    value_weight,
    output_weight,
    saved_output,
    norm_offset,
    output_grad,
):
    tp, sp = lax.axis_size("tp"), lax.axis_size("sp")
    Z, Y = sp // 2, tp // 2
    model, width = query_weight.shape
    heads = width // HEAD_DIM
    rows, srows = target_rows.shape[0], source_rows.shape[0]
    block = rows * tp
    count = block * sp
    source_count = srows * tp
    shift_base = math.log(source_count * sp)
    slice_width = model // sp
    dma = pltpu.SemaphoreType.DMA

    vm = pltpu.VMEM
    whole = pl.BlockSpec(memory_space=pl.ANY)
    flat_all, source_grad, target_grad, cols_all = pl.pallas_call(
        functools.partial(layer_kernel, sp, tp, shift_base),
        out_shape=[
            jax.ShapeDtypeStruct((sp, block, width), BF),
            jax.ShapeDtypeStruct((srows, model), F32),
            jax.ShapeDtypeStruct((rows, model), F32),
            jax.ShapeDtypeStruct((sp, tp, rows, slice_width), BF),
        ],
        in_specs=[VMEM] * 6 + [whole] * 4,
        out_specs=[VMEM] * 4,
        scratch_shapes=[vm((rows, model), BF), vm((sp, rows, slice_width), BF)]
        + [vm((model, width), BF)] * 3
        + [vm((width, model), BF)]
        + [vm((tp, rows, model), BF)] * 2
        + [vm((tp, srows, model), BF), vm((sp, rows, slice_width), BF)]
        + [vm((block, model), BF)] * 2
        + [vm((sp, block, width), BF)] * 2
        + [vm((sp, block, 128), BF)]
        + [vm((source_count, width), BF)] * 2
        + [vm((heads, count, source_count), BF)] * 2
        + [vm((sp, block, width), BF)]
        + [vm((source_count, width), BF)] * 2
        + [vm((tp, srows, model), BF)]
        + [vm((Z, block, width), BF)] * 3
        + [vm((Y, srows, model), BF)] * 3
        + [vm((tp, rows, model), BF)]
        + [vm((Y, rows, model), BF)] * 3
        + [dma((4,)), dma((5,)), dma((sp,)), dma((sp,))]
        + [dma((Y,))] * 24
        + [dma((Z,))] * 4
        + line_sems(Z, 3)
        + line_sems(Z, 1),
        name="layer_kernel",
        compiler_params=pltpu.CompilerParams(
            collective_id=1, has_side_effects=True, vmem_limit_bytes=58 * 2**20
        ),
    )(
        target_rows,
        output_grad,
        source_rows,
        norm_gain.reshape(1, model),
        saved_output,
        norm_offset.T,
        query_weight,
        key_weight,
        value_weight,
        output_weight,
    )
    weight_grad = lax.dot_general(
        cols_all.reshape(count, slice_width),
        flat_all.reshape(count, width),
        (((0,), (0,)), ((), ())),
        preferred_element_type=F32,
    )
    return (target_grad, source_grad, weight_grad)


def solution(mesh):
    in_specs = (
        P(("sp", "tp"), None),
        P(("sp", "tp"), None),
        P(),
        P(None, "tp"),
        P(None, "tp"),
        P(None, "tp"),
        P("tp", None),
        P("sp", "tp"),
        P("sp", "tp"),
        P(("sp", "tp"), None),
    )
    out_specs = (P(("sp", "tp"), None), P(("sp", "tp"), None), P("sp", "tp"))
    return jax.shard_map(body, mesh=mesh, in_specs=in_specs, out_specs=out_specs, check_vma=False)
```
